512 devices in a mesh: grp: 2 (over y), kv: 64 (over z, core), tp: 4 (over x).
Axes of the slice: x: 4, y: 2, z: 32, core: 2. Of those that a mesh axis runs over, the one named last changes fastest.
The devices are a block of a 4x8x32 slice.
Arguments:
- piece_rows: bfloat16 [8192, 2048], P(('grp', 'kv')), parts along dimension 0, may hold values from -6 to 6
- dec_rows: bfloat16 [256, 2048], P(('grp', 'kv')), parts along dimension 0, may hold values from -6 to 6
- norm_gain: float32 [2048], replicated, may hold values from 0.1 to 1.9
- w_query: bfloat16 [2048, 1024], P(None, 'tp'), may hold values from -0.25 to 0.25
- w_key: bfloat16 [2048, 256], P(None, 'tp'), may hold values from -0.125 to 0.125
- w_value: bfloat16 [2048, 256], P(None, 'tp'), may hold values from -0.125 to 0.125
- w_forget: bfloat16 [2048, 16], P(None, 'tp'), may hold values from -0.125 to 0.125
- forget_bias: float32 [16], P('tp'), may hold values from 3 to 12
- piece_decay: float32 [16, 8192], P('tp', ('grp', 'kv')), parts along dimension 1, may hold values from -3 to 0
- cache_kv: bfloat16 [98304, 4, 128], P(('grp', 'kv'), 'tp'), parts along dimension 0, may hold values from -150 to 150
- cache_gate: float32 [16, 98304], P('tp', ('grp', 'kv')), parts along dimension 1, may hold values from -2460.6 to 0, as said below
- dec_cache: bfloat16 [256, 3072, 4, 128], P(('grp', 'kv'), None, 'tp'), parts along dimension 0, may hold values from -150 to 150
- dec_gate: float32 [256, 16, 3072], P(('grp', 'kv'), 'tp'), parts along dimension 0, may hold values from -156.6 to 0, as said below
- dec_lengths: int32 [256], P(('grp', 'kv')), parts along dimension 0, may hold values from 1 to 3072, as said below
- w_out: bfloat16 [1024, 2048], P(None, 'tp'), may hold values from -0.75 to 0.75
Outputs:
- piece_out: bfloat16 [8192, 2048], P(('grp', 'kv'), 'tp'), parts along dimension 0
- dec_out: bfloat16 [256, 2048], P(('grp', 'kv'), 'tp'), parts along dimension 0
The draws below stay inside these ranges and needn't reach their ends.
There are 2 independent parts, one for each index of `grp`. The reference program is written for one: setup_inputs(seed, part) draws one part's arguments, and reference() takes and returns one part's arrays. A program takes and returns all parts, laid end to end along the dimension named above; an argument that names none is the same for every part. Nothing has to cross between parts.
Inputs may be any that keep to these rules, and one draw needn't show every extreme that they name: `cache_gate`: each head's values never fall from one position to the next and are 0 at the last cached position. `dec_gate`: each sequence's and head's values never rise from one position to the next. Sequence b's cache holds its first dec_lengths[b] positions; in each part some sequence holds 3072.
All inputs are finite; a program needn't handle non-finite values.
Results may differ from the reference program's by a relative error of at most 0.006.
The reference program's roundings to bfloat16 on the way count: a program that leaves them out, or rounds other values in their place, can miss the bound.
Values may be sent and summed in bfloat16 or wider, within the bound.
No kernel may reach another device: no remote copies, remote signals or barrier semaphores. Data moves between devices by JAX's collectives and lax.ppermute only.
A program may use at most 64 MiB of HBM per device.

```python
import math
import jax
import jax.numpy as jnp
from jax import lax

D = 2048
HEADS = 16
KV_HEADS = 4
HEAD_DIM = 64
PIECE_DEV = 64
PAST_DEV = 768
DEC_LEN = 3072
PIECE = 4096
PAST = 49152
DEC_SEQS = 128
N_KV = 64


def slow_heads(key, shape):
    pick = jax.random.randint(key, shape, 0, 10)
    return pick < 5


def gate_logs(key, rows, span, blocks):
    gradual_heads = slow_heads(jax.random.fold_in(key, 1), (rows, 1))
    factor = jnp.exp(jax.random.uniform(jax.random.fold_in(key, 2), (rows, blocks), jnp.float32, math.log(0.4), math.log(2.5)))
    factor = jnp.repeat(factor, span // blocks, axis=1)
    gradual_decay_rate = jax.random.uniform(jax.random.fold_in(key, 3), (rows, span), jnp.float32, 0.2, 1.0) * factor / span
    quick_decay_rate = jax.random.uniform(jax.random.fold_in(key, 4), (rows, span), jnp.float32, 0.01, 0.05)
    chosen_locations = jax.random.randint(jax.random.fold_in(key, 5), (rows, 3), 0, span)
    layer_depth = jax.random.uniform(jax.random.fold_in(key, 6), (rows, 3), jnp.float32, 0.22, 0.7)
    target_location = jnp.arange(span, dtype=jnp.int32)
    sudden_spike = jnp.sum(jnp.where(target_location[None, None, :] == chosen_locations[:, :, None], layer_depth[:, :, None], 0.0), axis=1)
    return -jnp.where(gradual_heads, gradual_decay_rate + sudden_spike, quick_decay_rate)


def spiky(key, shape):
    base = jnp.clip(jax.random.normal(jax.random.fold_in(key, 1), shape, jnp.float32), -6.0, 6.0)
    return base.astype(jnp.bfloat16)


def draw_forget_bias(key, part):
    gradual_heads = slow_heads(jax.random.fold_in(key, 11), (HEADS,))
    slow_value = jax.random.uniform(jax.random.fold_in(key, 12), (HEADS,), jnp.float32, 10.0, 12.0)
    fast_value = jax.random.uniform(jax.random.fold_in(key, 13), (HEADS,), jnp.float32, 3.0, 4.5)
    return jnp.where(gradual_heads, slow_value, fast_value)


def draw_piece_decay(key, part):
    decay_rates = jnp.exp(jax.random.uniform(jax.random.fold_in(key, 21), (N_KV,), jnp.float32, math.log(0.0002), math.log(0.003)))
    decay_rates = jnp.repeat(decay_rates, PIECE_DEV)
    random_noise = jax.random.uniform(jax.random.fold_in(key, 22), (HEADS, PIECE), jnp.float32, 0.5, 1.5)
    chosen_locations = jax.random.randint(jax.random.fold_in(key, 23), (3,), 0, PIECE)
    layer_depth = jax.random.uniform(jax.random.fold_in(key, 24), (HEADS, 3), jnp.float32, 0.22, 0.7)
    target_location = jnp.arange(PIECE, dtype=jnp.int32)
    sudden_spike = jnp.sum(jnp.where(target_location[None, None, :] == chosen_locations[None, :, None], layer_depth[:, :, None], 0.0), axis=1)
    return -(decay_rates[None, :] * random_noise + sudden_spike)


def draw_cache_gate(key, part):
    logs = gate_logs(jax.random.fold_in(key, 31), HEADS, PAST, N_KV)
    return jnp.flip(jnp.cumsum(jnp.flip(logs, 1), axis=1), 1) - logs


def draw_dec_gate(key, part):
    logs = gate_logs(jax.random.fold_in(key, 41), DEC_SEQS * HEADS, DEC_LEN, 1)
    return jnp.cumsum(logs, axis=1).reshape(DEC_SEQS, HEADS, DEC_LEN)


def draw_cache_kv(key, part):
    return spiky(jax.random.fold_in(key, 51), (PAST, KV_HEADS, 2 * HEAD_DIM))


def draw_dec_cache(key, part):
    return spiky(jax.random.fold_in(key, 61), (DEC_SEQS, DEC_LEN, KV_HEADS, 2 * HEAD_DIM))


def draw_dec_lengths(key, part):
    base = jax.random.randint(jax.random.fold_in(key, 71), (DEC_SEQS,), 1, DEC_LEN + 1)
    fullest = jax.random.randint(jax.random.fold_in(key, 72), (), 0, DEC_SEQS)
    slot_index = jnp.arange(DEC_SEQS, dtype=jnp.int32)
    return jnp.where(slot_index == fullest, DEC_LEN, base).astype(jnp.int32)


def level_of(key, shape, pieces, low, high):
    level = 1.0
    for dim, blocks in pieces:
        steps = jax.random.uniform(jax.random.fold_in(jax.random.fold_in(key, 6), dim), (blocks,), jnp.float32, low / len(pieces), high / len(pieces))
        level = level * jnp.repeat(jnp.exp(steps), shape[dim] // blocks).reshape((-1,) + (1,) * (len(shape) - 1 - dim))
    return level


def scatter_about(stream_key, dims, spread, most, pieces=(), held_as=jnp.bfloat16):
    result = spread * jax.random.normal(stream_key, dims, jnp.float32)
    if pieces:
        result = result * level_of(stream_key, dims, pieces, -0.22, 0.18)
    return jnp.clip(result, -most, most).astype(held_as)


def setup_inputs(seed: int = 0, part: int = 0) -> dict:
    key_of = jax.random.split(jax.random.key(seed), 16)
    own_keys = jax.random.split(jax.random.fold_in(key_of[15], part), 16)
    piece_rows = scatter_about(own_keys[0], (PIECE, D), 1.0, 6.0, ((0, 64),))
    dec_rows = scatter_about(own_keys[1], (DEC_SEQS, D), 1.0, 6.0, ((0, 64),))
    norm_gain = jnp.clip(1.0 + 0.18 * jax.random.normal(key_of[2], (D,), jnp.float32), 0.1, 1.9)
    w_query = scatter_about(key_of[3], (D, HEADS * HEAD_DIM), (D // 4) ** -0.5, 0.25, ((1, 4),))
    w_key = scatter_about(key_of[4], (D, KV_HEADS * HEAD_DIM), D ** -0.5, 0.125, ((1, 4),))
    w_value = scatter_about(key_of[5], (D, KV_HEADS * HEAD_DIM), D ** -0.5, 0.125, ((1, 4),))
    w_forget = scatter_about(key_of[6], (D, HEADS), D ** -0.5, 0.125, ((1, 4),))
    forget_bias = draw_forget_bias(jax.random.fold_in(key_of[15], 71), part)
    piece_decay = draw_piece_decay(jax.random.fold_in(jax.random.fold_in(key_of[15], part), 71), part)
    cache_kv = draw_cache_kv(jax.random.fold_in(jax.random.fold_in(key_of[15], part), 71), part)
    cache_gate = draw_cache_gate(jax.random.fold_in(jax.random.fold_in(key_of[15], part), 71), part)
    dec_cache = draw_dec_cache(jax.random.fold_in(jax.random.fold_in(key_of[15], part), 71), part)
    dec_gate = draw_dec_gate(jax.random.fold_in(jax.random.fold_in(key_of[15], part), 71), part)
    dec_lengths = draw_dec_lengths(jax.random.fold_in(jax.random.fold_in(key_of[15], part), 71), part)
    w_out = scatter_about(key_of[14], (HEADS * HEAD_DIM, D), HEAD_DIM ** -0.5, 0.75, ((1, 4),))
    return dict(piece_rows=piece_rows, dec_rows=dec_rows, norm_gain=norm_gain, w_query=w_query, w_key=w_key, w_value=w_value, w_forget=w_forget, forget_bias=forget_bias, piece_decay=piece_decay, cache_kv=cache_kv, cache_gate=cache_gate, dec_cache=dec_cache, dec_gate=dec_gate, dec_lengths=dec_lengths, w_out=w_out)


def norm_rows(rows, gain):
    wide = rows.astype(jnp.float32)
    scale = lax.rsqrt(lax.optimization_barrier(jnp.mean(wide * wide, axis=-1, keepdims=True)) + 1e-06)
    return (wide * scale * gain.astype(jnp.float32)).astype(jnp.bfloat16)

def merge_state(state, part):
    peak, total, numer = state
    new_peak, new_total, new_numer = part
    highest = jnp.maximum(peak, new_peak)
    keep = jnp.exp(peak - highest)
    fresh = jnp.exp(new_peak - highest)
    return (highest, total * keep + new_total * fresh, numer * keep[..., None] + new_numer * fresh[..., None])

def group_partial(query, query_index, group_kv, group_bias, group, past_rows, new_rows):
    head_width = query.shape[-1]
    keys = group_kv[..., :head_width].astype(jnp.float32)
    values = group_kv[..., head_width:].astype(jnp.float32)
    score = jnp.einsum('bkgd,nkd->bkgn', query.astype(jnp.float32), keys)
    score = score * head_width ** (-0.5) + group_bias[None]
    rank = jnp.arange(group_kv.shape[0], dtype=jnp.int32)
    new_index = group * new_rows + rank - past_rows
    visible = (rank < past_rows)[None, :] | (new_index[None, :] <= query_index[:, None])
    score = jnp.where(visible[:, None, None, :], score, -jnp.inf)
    peak = lax.optimization_barrier(jnp.max(score, axis=-1))
    weight = jnp.exp(score - peak[..., None])
    total = lax.optimization_barrier(jnp.sum(weight, axis=-1))
    rounded = lax.optimization_barrier(weight.astype(jnp.bfloat16))
    numer = jnp.einsum('bkgn,nkd->bkgd', rounded.astype(jnp.float32), values)
    return (peak, total, numer)

def decode_attention(query, new_key, new_value, new_gate, cache, gate, lengths):
    seqs, pairs_here, group_size, head_width = query.shape
    span = cache.shape[1]
    keys = cache[..., :head_width].astype(jnp.float32)
    values = cache[..., head_width:].astype(jnp.float32)
    target_location = jnp.arange(span, dtype=jnp.int32)
    last_gate = lax.optimization_barrier(jnp.sum(jnp.where(target_location[None, None, :] == lengths[:, None, None] - 1, gate, 0.0), axis=-1))
    score = jnp.einsum('skgd,slkd->skgl', query.astype(jnp.float32), keys) * head_width ** (-0.5)
    score = score - gate.reshape(seqs, pairs_here, group_size, span)
    score = jnp.where((target_location[None, :] < lengths[:, None])[:, None, None, :], score, -jnp.inf)
    own = jnp.einsum('skgd,skd->skg', query.astype(jnp.float32), new_key.astype(jnp.float32)) * head_width ** (-0.5)
    own = own - (last_gate + new_gate).reshape(seqs, pairs_here, group_size)
    peak = jnp.maximum(lax.optimization_barrier(jnp.max(score, axis=-1)), own)
    weight = jnp.exp(score - peak[..., None])
    own_weight = jnp.exp(own - peak)
    total = lax.optimization_barrier(jnp.sum(weight, axis=-1)) + own_weight
    rounded = lax.optimization_barrier(weight.astype(jnp.bfloat16))
    own_rounded = lax.optimization_barrier(own_weight.astype(jnp.bfloat16))
    numer = jnp.einsum('skgl,slkd->skgd', rounded.astype(jnp.float32), values)
    numer = numer + own_rounded.astype(jnp.float32)[..., None] * new_value[:, :, None, :].astype(jnp.float32)
    return numer / total[..., None]

def reference(piece_rows, dec_rows, norm_gain, w_query, w_key, w_value, w_forget, forget_bias, piece_decay, cache_kv, cache_gate, dec_cache, dec_gate, dec_lengths, w_out):
    group_size = HEADS // KV_HEADS
    normed = norm_rows(jnp.concatenate([piece_rows, dec_rows], axis=0), norm_gain)
    query = jnp.dot(normed, w_query, preferred_element_type=jnp.float32).astype(jnp.bfloat16)
    new_key = jnp.dot(normed, w_key, preferred_element_type=jnp.float32).astype(jnp.bfloat16)
    new_value = jnp.dot(normed, w_value, preferred_element_type=jnp.float32).astype(jnp.bfloat16)
    log_gate = jax.nn.log_sigmoid(jnp.dot(normed, w_forget, preferred_element_type=jnp.float32) + forget_bias)
    piece_gate = log_gate[:PIECE] + piece_decay.T
    new_bias = -jnp.cumsum(piece_gate, axis=0).T
    piece_kv = jnp.concatenate([new_key[:PIECE].reshape(PIECE, KV_HEADS, HEAD_DIM), new_value[:PIECE].reshape(PIECE, KV_HEADS, HEAD_DIM)], axis=-1)
    past_groups = cache_kv.reshape(N_KV, PAST_DEV, KV_HEADS, 2 * HEAD_DIM)
    new_groups = piece_kv.reshape(N_KV, PIECE_DEV, KV_HEADS, 2 * HEAD_DIM)
    past_bias = jnp.transpose(cache_gate.reshape(HEADS, N_KV, PAST_DEV), (1, 0, 2))
    fresh_bias = jnp.transpose(new_bias.reshape(HEADS, N_KV, PIECE_DEV), (1, 0, 2))
    all_query = query[:PIECE].reshape(PIECE, KV_HEADS, group_size, HEAD_DIM)
    query_index = jnp.arange(PIECE, dtype=jnp.int32)

    def visit(state, item):
        past, fresh, past_gate, fresh_gate, group = item
        block = jnp.concatenate([past, fresh], axis=0)
        bias = jnp.concatenate([past_gate, fresh_gate], axis=1).reshape(KV_HEADS, group_size, PAST_DEV + PIECE_DEV)
        part = group_partial(all_query, query_index, block, bias, group, PAST_DEV, PIECE_DEV)
        return (merge_state(state, part), None)
    start_state = (jnp.full((PIECE, KV_HEADS, group_size), -jnp.inf, jnp.float32), jnp.zeros((PIECE, KV_HEADS, group_size), jnp.float32), jnp.zeros((PIECE, KV_HEADS, group_size, HEAD_DIM), jnp.float32))
    state, _ = lax.scan(visit, start_state, (past_groups, new_groups, past_bias, fresh_bias, jnp.arange(N_KV, dtype=jnp.int32)))
    piece_attn = (state[2] / state[1][..., None]).reshape(PIECE, HEADS * HEAD_DIM).astype(jnp.bfloat16)
    dec_count = dec_rows.shape[0]
    dec_attn = decode_attention(query[PIECE:].reshape(dec_count, KV_HEADS, group_size, HEAD_DIM), new_key[PIECE:].reshape(dec_count, KV_HEADS, HEAD_DIM), new_value[PIECE:].reshape(dec_count, KV_HEADS, HEAD_DIM), log_gate[PIECE:], dec_cache, dec_gate, dec_lengths)
    dec_attn = dec_attn.reshape(dec_count, HEADS * HEAD_DIM).astype(jnp.bfloat16)
    piece_out = jnp.dot(piece_attn, w_out, preferred_element_type=jnp.float32).astype(jnp.bfloat16)
    dec_out = jnp.dot(dec_attn, w_out, preferred_element_type=jnp.float32).astype(jnp.bfloat16)
    return (piece_out, dec_out)
```

```python
import jax
import jax.numpy as jnp
from jax import lax
from jax.experimental import pallas as pl
from jax.experimental.pallas import tpu as pltpu
from jax.sharding import Mesh
from jax.sharding import PartitionSpec as P

KV = ("kv_0", "kv_1")
GRP_KV = ("grp", "kv_0", "kv_1")


def carried_in(array, axis, combine, identity):
    length, mine = (lax.axis_size(axis), lax.axis_index(axis))
    everything = lax.all_gather(array, axis)
    start = jnp.broadcast_to(jnp.asarray(identity, array.dtype), array.shape)

    def lap(k, before):
        reached = k < mine
        new = combine(before, everything[k])
        return jnp.where(reached, new, before)

    return lax.fori_loop(0, length, lap, start)


def in_order(blocks, dim):
    blocks = jnp.moveaxis(blocks, 0, dim)
    lengths = blocks.shape
    return blocks.reshape(*lengths[:dim], lengths[dim] * lengths[dim + 1], *lengths[dim + 2 :])


def stacked_from(array, axes, turns):
    blocks = array
    for k in turns:
        blocks = lax.all_gather(blocks, axes[k])
    done = turns[::-1]
    back = [done.index(k) for k in range(len(axes))]
    blocks = blocks.transpose(*back, *range(len(axes), blocks.ndim))
    return blocks.reshape(-1, *array.shape)


def whole_of(array, axes, turns, dim):
    return in_order(stacked_from(array, axes, turns), dim)


def sent_to_all(array, axis):
    length = lax.axis_size(axis)
    return lax.all_to_all(
        jnp.broadcast_to(array[None], (length, *array.shape)), axis, 0, 0, tiled=True
    )


def gathered_copies(array, axis, dim):
    blocks = sent_to_all(array, axis)
    return in_order(blocks, dim)


def norm_rows(rows, gain):
    wide = rows.astype(jnp.float32)
    scale = lax.rsqrt(jnp.mean(wide * wide, axis=-1, keepdims=True) + 1e-06)
    return (wide * scale * gain).astype(jnp.bfloat16)


def add_terms(earlier, later):
    return earlier + later


def absorb(state, score, values):
    peak, acc = state
    highest = jnp.maximum(peak, jnp.max(score, axis=0, keepdims=True))
    weight = jnp.exp(score - highest).astype(jnp.bfloat16)
    fresh = jnp.dot(values, weight, preferred_element_type=jnp.float32)
    return highest, acc * jnp.exp(peak - highest) + fresh


def operands(rows, bias):
    count, width = rows.shape
    half = width // 2
    pieces = bias.shape[0]
    wide = jnp.concatenate(
        [
            jnp.zeros((half, count), jnp.bfloat16),
            bias,
            jnp.zeros((half - pieces, count), jnp.bfloat16),
        ],
        axis=0,
    )
    lane = lax.broadcasted_iota(jnp.int32, (count, width), 1)
    keys = jnp.where(lane < half, rows, wide.T)
    values = jnp.concatenate([rows.T[half:], jnp.ones((16, count), jnp.bfloat16)], axis=0)
    return keys, values


def flash_kernel(base_ref, q_ref, index_ref, kv_ref, bias_ref, fresh_ref, fresh_bias_ref, peak_ref, acc_ref):
    step = pl.program_id(1)
    query = q_ref[...]

    @pl.when(step == 0)
    def _():
        peak_ref[...] = jnp.full_like(peak_ref, -jnp.inf)
        acc_ref[...] = jnp.zeros_like(acc_ref)

    state = peak_ref[...], acc_ref[...]
    for k in range(kv_ref.shape[0]):
        keys, values = operands(kv_ref[k], bias_ref[k])
        score = jnp.dot(keys, query, preferred_element_type=jnp.float32)
        state = absorb(state, score, values)
    peak_ref[...], acc_ref[...] = state

    @pl.when(step == pl.num_programs(1) - 1)
    def _():
        chunks, count, _ = fresh_ref.shape

        def visit(k, state):
            keys, values = operands(fresh_ref[k], fresh_bias_ref[k])
            score = jnp.dot(keys, query, preferred_element_type=jnp.float32)
            place = base_ref[0] + k * count + lax.broadcasted_iota(jnp.int32, score.shape, 0)
            score = jnp.where(place <= index_ref[...], score, -jnp.inf)
            return absorb(state, score, values)

        peak_ref[...], acc_ref[...] = lax.fori_loop(0, chunks, visit, (peak_ref[...], acc_ref[...]))


def flash(base, query, index, kv, bias, fresh, fresh_bias, past_rows, at_once, tile):
    width, rows = query.shape
    shards = kv.shape[0]
    half = width // 2
    whole = lambda array: pl.BlockSpec(array.shape, lambda r, s: (0,) * array.ndim)
    return pl.pallas_call(
        flash_kernel,
        grid=(rows // tile, shards // at_once),
        in_specs=[
            pl.BlockSpec(memory_space=pltpu.SMEM),
            pl.BlockSpec((width, tile), lambda r, s: (0, r)),
            pl.BlockSpec((1, tile), lambda r, s: (0, r)),
            pl.BlockSpec((at_once, past_rows, width), lambda r, s: (s, 0, 0)),
            pl.BlockSpec((at_once, *bias.shape[1:]), lambda r, s: (s, 0, 0)),
            whole(fresh),
            whole(fresh_bias),
        ],
        out_specs=[
            pl.BlockSpec((1, tile), lambda r, s: (0, r)),
            pl.BlockSpec((half + 16, tile), lambda r, s: (0, r)),
        ],
        out_shape=[
            jax.ShapeDtypeStruct((1, rows), jnp.float32),
            jax.ShapeDtypeStruct((half + 16, rows), jnp.float32),
        ],
        compiler_params=pltpu.CompilerParams(
            dimension_semantics=("arbitrary", "arbitrary"), vmem_limit_bytes=48 * 2**20
        ),
        name="flash",
    )(base, query, index, kv, bias, fresh, fresh_bias)


def bf16_pieces(array, dim):
    first = lax.reduce_precision(array, 8, 7)
    left = array - first
    second = lax.reduce_precision(left, 8, 7)
    pieces = [first, second, left - second, jnp.zeros_like(first)]
    return jnp.concatenate(pieces, axis=dim).astype(jnp.bfloat16)


def head_rows(query, tile_heads):
    positions = query.shape[0]
    width = query.shape[1] // tile_heads
    turned = query.reshape(positions, tile_heads, width).transpose(2, 1, 0).reshape(width, -1)
    turned = turned * jnp.asarray(width ** (-0.5), query.dtype)
    head = jnp.arange(tile_heads * positions, dtype=jnp.int32) // positions
    row = jnp.arange(width, dtype=jnp.int32)
    pick = (row[:, None] % tile_heads == head[None, :]) & (row[:, None] < 3 * tile_heads)
    return jnp.concatenate([turned, pick.astype(query.dtype)], axis=0)


def decode_attention(query, new_key, new_value, new_gate, cache, gate, lengths):
    seqs, pairs_here, group_size, head_width = query.shape
    span = cache.shape[1]
    keys = cache[..., :head_width]
    values = cache[..., head_width:]
    target_location = jnp.arange(span, dtype=jnp.int32)
    last_gate = jnp.sum(
        jnp.where(target_location[None, None, :] == lengths[:, None, None] - 1, gate, 0.0), axis=-1
    )
    score = jnp.einsum(
        "skgd,slkd->skgl", query, keys, preferred_element_type=jnp.float32
    ) * head_width ** (-0.5)
    score = score - gate.reshape(seqs, pairs_here, group_size, span)
    score = jnp.where(
        (target_location[None, :] < lengths[:, None])[:, None, None, :], score, -jnp.inf
    )
    own = jnp.einsum(
        "skgd,skd->skg", query, new_key, preferred_element_type=jnp.float32
    ) * head_width ** (-0.5)
    own = own - (last_gate + new_gate).reshape(seqs, pairs_here, group_size)
    peak = jnp.maximum(jnp.max(score, axis=-1), own)
    weight = jnp.exp(score - peak[..., None])
    own_weight = jnp.exp(own - peak)
    total = jnp.sum(weight, axis=-1) + own_weight
    numer = jnp.einsum(
        "skgl,slkd->skgd", weight.astype(jnp.bfloat16), values, preferred_element_type=jnp.float32
    )
    numer = numer + own_weight.astype(jnp.bfloat16).astype(jnp.float32)[..., None] * new_value[
        :, :, None, :
    ].astype(jnp.float32)
    return numer / total[..., None]


def local(
    piece_rows,
    dec_rows,
    norm_gain,
    w_query,
    w_key,
    w_value,
    w_forget,
    forget_bias,
    piece_decay,
    cache_kv,
    cache_gate,
    dec_cache,
    dec_gate,
    dec_lengths,
    w_out,
):
    piece_count = piece_rows.shape[0]
    dec_count = dec_rows.shape[0]
    past_rows = cache_kv.shape[0]
    pairs_here = cache_kv.shape[1]
    head_width = cache_kv.shape[2] // 2
    heads_here = w_forget.shape[1]
    group_size = heads_here // pairs_here
    group_rows = past_rows + piece_count
    normed = norm_rows(jnp.concatenate([piece_rows, dec_rows], axis=0), norm_gain)
    query = jnp.dot(normed, w_query, preferred_element_type=jnp.float32).astype(jnp.bfloat16)
    new_key = jnp.dot(normed, w_key, preferred_element_type=jnp.float32).astype(jnp.bfloat16)
    new_value = jnp.dot(normed, w_value, preferred_element_type=jnp.float32).astype(jnp.bfloat16)
    log_gate = jax.nn.log_sigmoid(
        jnp.dot(normed, w_forget, preferred_element_type=jnp.float32) + forget_bias
    )
    piece_gate = log_gate[:piece_count] + piece_decay.T
    running = jnp.cumsum(piece_gate, axis=0)
    before = carried_in(running[-1], KV, add_terms, jnp.zeros((heads_here,), jnp.float32))
    new_bias = -(running + before[None, :]).T
    piece_kv = jnp.concatenate(
        [
            new_key[:piece_count].reshape(piece_count, pairs_here, head_width),
            new_value[:piece_count].reshape(piece_count, pairs_here, head_width),
        ],
        axis=-1,
    )
    group_kv = jnp.concatenate([cache_kv, piece_kv], axis=0)
    group_bias = jnp.concatenate([cache_gate, new_bias], axis=1)
    my_group = lax.axis_index(KV)
    every_bias = stacked_from(group_bias, KV, (0, 1))
    gathered = lax.all_gather(group_kv, KV, axis=0, tiled=True)
    shards = gathered.shape[0] // group_rows
    gathered = gathered.reshape(shards, group_rows, 2 * head_width)
    joined = 4
    chunk = joined * piece_count
    fresh_bias = every_bias[:, :, past_rows:].reshape(shards // joined, joined, heads_here, piece_count)
    fresh_bias = fresh_bias.transpose(0, 2, 1, 3).reshape(shards // joined, heads_here, chunk)
    place = my_group * piece_count + jnp.arange(piece_count, dtype=jnp.int32)
    peak, acc = flash(
        jnp.zeros((1,), jnp.int32),
        head_rows(query[:piece_count], heads_here),
        jnp.tile(place, heads_here)[None],
        gathered,
        bf16_pieces(every_bias[:, :, :past_rows], 1),
        gathered[:, past_rows:].reshape(shards // joined, chunk, 2 * head_width),
        bf16_pieces(fresh_bias, 1),
        past_rows,
        joined,
        heads_here * piece_count,
    )
    piece_attn = acc[:head_width] / acc[head_width : head_width + 1]
    piece_attn = piece_attn.reshape(head_width, heads_here, piece_count).transpose(2, 1, 0)
    dec_attn = decode_attention(
        query[piece_count:].reshape(dec_count, pairs_here, group_size, head_width),
        new_key[piece_count:].reshape(dec_count, pairs_here, head_width),
        new_value[piece_count:].reshape(dec_count, pairs_here, head_width),
        log_gate[piece_count:],
        dec_cache,
        dec_gate,
        dec_lengths,
    )
    attn_rows = jnp.concatenate(
        [
            piece_attn.reshape(piece_count, heads_here * head_width),
            dec_attn.reshape(dec_count, heads_here * head_width),
        ],
        axis=0,
    ).astype(jnp.bfloat16)
    every_head = gathered_copies(attn_rows, "tp", 1)
    mixed = jnp.dot(every_head, w_out, preferred_element_type=jnp.float32).astype(jnp.bfloat16)
    return (mixed[:piece_count], mixed[piece_count:])


def solution(mesh):
    finer = Mesh(
        mesh.devices.reshape(mesh.shape["grp"], 32, 2, mesh.shape["tp"]),
        ("grp", "kv_0", "kv_1", "tp"),
    )
    return jax.shard_map(
        local,
        mesh=finer,
        in_specs=(
            P(GRP_KV, None),
            P(GRP_KV, None),
            P(),
            P(None, "tp"),
            P(None, "tp"),
            P(None, "tp"),
            P(None, "tp"),
            P("tp"),
            P("tp", GRP_KV),
            P(GRP_KV, "tp", None),
            P("tp", GRP_KV),
            P(GRP_KV, None, "tp", None),
            P(GRP_KV, "tp", None),
            P(GRP_KV),
            P(None, "tp"),
        ),
        out_specs=(P(GRP_KV, "tp"), P(GRP_KV, "tp")),
        check_vma=False,
    )
```

```python
import functools

import jax
import jax.numpy as jnp
from jax import lax
from jax.experimental import pallas as pl
from jax.experimental.pallas import tpu as pltpu
from jax.sharding import Mesh
from jax.sharding import PartitionSpec as P

GRP_KV = ("grp", "run", "near", "core")
PIECES = 3
SPARE = 8


def to_each(array, axis):
    members = lax.axis_size(axis)
    return lax.all_to_all(
        jnp.broadcast_to(array[None], (members, *array.shape)), axis, 0, 0, tiled=True
    )


def norm_rows(rows, gain):
    wide = rows.astype(jnp.float32)
    scale = lax.rsqrt(jnp.mean(wide * wide, axis=-1, keepdims=True) + 1e-06)
    return (wide * scale * gain).astype(jnp.bfloat16)


def absorb(state, score, values):
    peak, acc = state
    highest = jnp.maximum(peak, jnp.max(score, axis=0, keepdims=True))
    weight = jnp.exp(score - highest).astype(jnp.bfloat16)
    fresh = jnp.dot(values, weight, preferred_element_type=jnp.float32)
    return highest, acc * jnp.exp(peak - highest) + fresh


def operands(rows, bias):
    count, width = rows.shape
    half = width // 2
    pieces = bias.shape[0]
    wide = jnp.concatenate(
        [
            jnp.zeros((half, count), jnp.bfloat16),
            bias,
            jnp.zeros((half - pieces, count), jnp.bfloat16),
        ],
        axis=0,
    )
    lane = lax.broadcasted_iota(jnp.int32, (count, width), 1)
    keys = jnp.where(lane < half, rows, wide.T)
    values = jnp.concatenate([rows.T[half:], jnp.ones((16, count), jnp.bfloat16)], axis=0)
    return keys, values


def cut(array):
    first = array.astype(jnp.bfloat16).astype(jnp.float32)
    left = array - first
    second = left.astype(jnp.bfloat16).astype(jnp.float32)
    return [first, second, left - second]


def query_tile(q_ref, first_head, heads):
    members, width, lanes = q_ref.shape
    turned = jnp.concatenate([q_ref[k] for k in range(members)], axis=1)
    each = lanes // (heads // 2)
    shape = (width, members * lanes)
    row = lax.broadcasted_iota(jnp.int32, shape, 0)
    head = first_head + lax.broadcasted_iota(jnp.int32, shape, 1) % lanes // each
    pick = (row % heads == head) & (row < PIECES * heads)
    return jnp.concatenate([turned, pick.astype(jnp.float32).astype(jnp.bfloat16)], axis=0)


def past_kernel(first_head, heads, q_ref, mine_ref, other_ref, mine_bias_ref, other_bias_ref, peak_ref, acc_ref):
    query = query_tile(q_ref, first_head, heads)

    @pl.when(pl.program_id(1) == 0)
    def _():
        peak_ref[...] = jnp.full_like(peak_ref, -jnp.inf)
        acc_ref[...] = jnp.zeros_like(acc_ref)

    state = peak_ref[...], acc_ref[...]
    for kv_ref, bias_ref in ((mine_ref, mine_bias_ref), (other_ref, other_bias_ref)):
        for k in range(kv_ref.shape[0]):
            keys, values = operands(kv_ref[k], bias_ref[k])
            score = jnp.dot(keys, query, preferred_element_type=jnp.float32)
            state = absorb(state, score, values)
    peak_ref[...], acc_ref[...] = state


def fresh_kernel(first_head, heads, place_ref, q_ref, kv_ref, bias_ref, peak_ref, acc_ref, out_ref):
    query = query_tile(q_ref, first_head, heads)
    width, tile = query.shape
    half = width // 2
    members, _, lanes = out_ref.shape
    each = lanes // (heads // 2)
    chunks, count, _ = kv_ref.shape
    state = peak_ref[...], acc_ref[...]
    lane = lax.broadcasted_iota(jnp.int32, (1, tile), 1)
    member = pl.program_id(0) * members + lane // lanes
    asked = member * (chunks * count) + place_ref[0] + lane % each
    for k in range(chunks):
        keys, values = operands(kv_ref[k], bias_ref[k])
        score = jnp.dot(keys, query, preferred_element_type=jnp.float32)
        place = place_ref[1] + k * count + lax.broadcasted_iota(jnp.int32, score.shape, 0)
        score = jnp.where(place <= asked, score, -jnp.inf)
        state = absorb(state, score, values)
    peak, acc = state
    rows = [acc[:half], *cut(peak), *cut(acc[half : half + 1])]
    rows.append(jnp.zeros((SPARE - 2 * PIECES, tile), jnp.float32))
    sent = jnp.concatenate(rows, axis=0).astype(jnp.bfloat16)
    for k in range(members):
        out_ref[k] = sent[:, k * lanes : (k + 1) * lanes]


def attend(side, places, queries, mine, other, mine_bias, other_bias, fresh, fresh_bias, past_rows, heads):
    members, _, lanes = queries.shape
    shards, _, width = mine.shape
    half = width // 2
    at_once, joined = 2, 2
    tile = joined * lanes
    rows = members * lanes
    whole = lambda array: pl.BlockSpec(array.shape, lambda *_: (0,) * array.ndim)
    shard = lambda count: pl.BlockSpec((at_once, count, width), lambda r, s: (s, 0, 0))
    bias_block = pl.BlockSpec((at_once, *mine_bias.shape[1:]), lambda r, s: (s, 0, 0))
    first_head = side * (heads // 2)
    work = 2 * shards * past_rows * rows
    peak, acc = pl.pallas_call(
        functools.partial(past_kernel, first_head, heads),
        grid=(members // joined, shards // at_once),
        in_specs=[
            pl.BlockSpec((joined, half, lanes), lambda r, s: (r, side, 0)),
            shard(past_rows),
            shard(past_rows),
            bias_block,
            bias_block,
        ],
        out_specs=[
            pl.BlockSpec((1, tile), lambda r, s: (0, r)),
            pl.BlockSpec((half + 16, tile), lambda r, s: (0, r)),
        ],
        out_shape=[
            jax.ShapeDtypeStruct((1, rows), jnp.float32),
            jax.ShapeDtypeStruct((half + 16, rows), jnp.float32),
        ],
        compiler_params=pltpu.CompilerParams(
            dimension_semantics=("arbitrary", "arbitrary"), vmem_limit_bytes=40 * 2**20
        ),
        cost_estimate=pl.CostEstimate(
            flops=work * width * 2, transcendentals=work, bytes_accessed=4 * mine.size
        ),
        name="past",
    )(queries, mine, other, mine_bias, other_bias)
    return pl.pallas_call(
        functools.partial(fresh_kernel, first_head, heads),
        grid=(members // joined,),
        in_specs=[
            pl.BlockSpec(memory_space=pltpu.SMEM),
            pl.BlockSpec((joined, half, lanes), lambda r: (r, side, 0)),
            whole(fresh),
            whole(fresh_bias),
            pl.BlockSpec((1, tile), lambda r: (0, r)),
            pl.BlockSpec((half + 16, tile), lambda r: (0, r)),
        ],
        out_specs=pl.BlockSpec((joined, half + SPARE, lanes), lambda r: (r, 0, 0)),
        out_shape=jax.ShapeDtypeStruct((members, half + SPARE, lanes), jnp.bfloat16),
        compiler_params=pltpu.CompilerParams(
            dimension_semantics=("arbitrary",), vmem_limit_bytes=32 * 2**20
        ),
        cost_estimate=pl.CostEstimate(
            flops=fresh.shape[0] * fresh.shape[1] * rows * width * 4,
            transcendentals=fresh.shape[0] * fresh.shape[1] * rows,
            bytes_accessed=4 * acc.size,
        ),
        name="fresh",
    )(places, queries, fresh, fresh_bias, peak, acc)


def bf16_pieces(array, dim):
    first = lax.reduce_precision(array, 8, 7)
    left = array - first
    second = lax.reduce_precision(left, 8, 7)
    return jnp.concatenate([first, second, left - second], axis=dim).astype(jnp.bfloat16)


def bias_rows(bias):
    pieces = bf16_pieces(bias, -2)
    spare = jnp.zeros((*pieces.shape[:-2], 16 - pieces.shape[-2], pieces.shape[-1]), jnp.bfloat16)
    return jnp.concatenate([pieces, spare], axis=-2)


def packed(array, lanes):
    flat = array.reshape(-1)
    rows = -(-flat.shape[0] // lanes)
    return jnp.pad(flat, (0, rows * lanes - flat.shape[0])).reshape(rows, lanes)


def merged(parts, half):
    wide = parts.astype(jnp.float32)
    peak = wide[:, half] + wide[:, half + 1] + wide[:, half + 2]
    total = wide[:, half + 3] + wide[:, half + 4] + wide[:, half + 5]
    share = jnp.exp(peak - jnp.max(peak, axis=0))
    numer = jnp.sum(wide[:, :half] * share[:, None, :], axis=0)
    return numer / jnp.sum(total * share, axis=0)


def decode_attention(query, new_key, new_value, new_gate, cache, gate, lengths):
    seqs, pairs_here, group_size, head_width = query.shape
    span = cache.shape[1]
    keys = cache[..., :head_width]
    values = cache[..., head_width:]
    target_location = jnp.arange(span, dtype=jnp.int32)
    last_gate = jnp.sum(
        jnp.where(target_location[None, None, :] == lengths[:, None, None] - 1, gate, 0.0), axis=-1
    )
    score = jnp.einsum(
        "skgd,slkd->skgl", query, keys, preferred_element_type=jnp.float32
    ) * head_width ** (-0.5)
    score = score - gate.reshape(seqs, pairs_here, group_size, span)
    score = jnp.where(
        (target_location[None, :] < lengths[:, None])[:, None, None, :], score, -jnp.inf
    )
    own = jnp.einsum(
        "skgd,skd->skg", query, new_key, preferred_element_type=jnp.float32
    ) * head_width ** (-0.5)
    own = own - (last_gate + new_gate).reshape(seqs, pairs_here, group_size)
    peak = jnp.maximum(jnp.max(score, axis=-1), own)
    weight = jnp.exp(score - peak[..., None])
    own_weight = jnp.exp(own - peak)
    total = jnp.sum(weight, axis=-1) + own_weight
    numer = jnp.einsum(
        "skgl,slkd->skgd", weight.astype(jnp.bfloat16), values, preferred_element_type=jnp.float32
    )
    numer = numer + own_weight.astype(jnp.bfloat16).astype(jnp.float32)[..., None] * new_value[
        :, :, None, :
    ].astype(jnp.float32)
    return numer / total[..., None]


def step(
    piece_rows,
    dec_rows,
    norm_gain,
    w_query,
    w_key,
    w_value,
    w_forget,
    forget_bias,
    piece_decay,
    cache_kv,
    cache_gate,
    dec_cache,
    dec_gate,
    dec_lengths,
    w_out,
):
    piece_count = piece_rows.shape[0]
    dec_count = dec_rows.shape[0]
    past_rows, pairs_here, width = cache_kv.shape
    head_width = width // 2
    heads_here = w_forget.shape[1]
    group_size = heads_here // pairs_here
    lanes = heads_here // 2 * piece_count
    neighbours = lax.axis_size(("near", "core"))
    me = lax.axis_index(("near", "core"))
    run = lax.axis_index("run")

    past_bias = bias_rows(cache_gate)
    past = jnp.concatenate([cache_kv[:, 0], past_bias.reshape(-1, width)], axis=0)
    mine = to_each(past, "near")

    normed = norm_rows(jnp.concatenate([piece_rows, dec_rows], axis=0), norm_gain)
    query = jnp.dot(normed, w_query, preferred_element_type=jnp.float32).astype(jnp.bfloat16)
    new_key = jnp.dot(normed, w_key, preferred_element_type=jnp.float32).astype(jnp.bfloat16)
    new_value = jnp.dot(normed, w_value, preferred_element_type=jnp.float32).astype(jnp.bfloat16)
    log_gate = jax.nn.log_sigmoid(
        jnp.dot(normed, w_forget, preferred_element_type=jnp.float32) + forget_bias
    )
    running = jnp.cumsum(log_gate[:piece_count].T + piece_decay, axis=1)

    scaled = query[:piece_count] * jnp.asarray(head_width ** (-0.5), query.dtype)
    turned = scaled.reshape(piece_count, 2, heads_here // 2, head_width).transpose(1, 3, 2, 0)
    asked = jnp.concatenate(
        [
            turned.reshape(2 * head_width, lanes),
            packed(bf16_pieces(running[None, :, -1], 0), lanes),
            jnp.zeros((SPARE - 1, lanes), jnp.bfloat16),
        ],
        axis=0,
    )
    asked, mine = lax.optimization_barrier((asked, mine))
    queries = to_each(asked, "run")
    other = lax.ppermute(mine, "core", [(0, 1), (1, 0)])
    mine_bias, other_bias = (
        block[:, past_rows:].reshape(-1, *past_bias.shape) for block in (mine, other)
    )
    totals = queries[:, 2 * head_width, : PIECES * heads_here].astype(jnp.float32)
    totals = totals.reshape(-1, PIECES, heads_here).sum(1)
    earlier = jnp.arange(totals.shape[0], dtype=jnp.int32)[:, None] < run
    earlier = jnp.sum(jnp.where(earlier, totals, 0.0), axis=0)

    own = jnp.concatenate(
        [
            jnp.concatenate([new_key[:piece_count], new_value[:piece_count]], axis=1),
            packed(bf16_pieces(running[None], 0), width),
            packed(bf16_pieces(earlier[None], 0), width),
        ],
        axis=0,
    )
    own = jnp.pad(own, ((0, -own.shape[0] % SPARE), (0, 0)))
    dec_attn = decode_attention(
        query[piece_count:].reshape(dec_count, pairs_here, group_size, head_width),
        new_key[piece_count:].reshape(dec_count, pairs_here, head_width),
        new_value[piece_count:].reshape(dec_count, pairs_here, head_width),
        log_gate[piece_count:],
        dec_cache,
        dec_gate,
        dec_lengths,
    )
    own, dec_attn = lax.optimization_barrier((own, dec_attn))
    news = to_each(own, ("near", "core"))
    run_rows = PIECES * heads_here * piece_count // width
    ran = news[:, piece_count : piece_count + run_rows].astype(jnp.float32)
    ran = ran.reshape(neighbours, PIECES, heads_here, piece_count).sum(1)
    before = news[:, piece_count + run_rows, : PIECES * heads_here].astype(jnp.float32)
    before = before.reshape(neighbours, PIECES, heads_here).sum((0, 1))
    ends = ran[:, :, -1]
    before = before + jnp.cumsum(ends, axis=0) - ends
    joined = 4
    chunks = neighbours // joined
    fresh_bias = -(ran + before[:, :, None])
    fresh_bias = fresh_bias.reshape(chunks, joined, heads_here, piece_count).transpose(0, 2, 1, 3)
    fresh_bias = bias_rows(fresh_bias.reshape(chunks, heads_here, joined * piece_count))
    fresh = news[:, :piece_count].reshape(chunks, joined * piece_count, width)
    places = jnp.stack([me, run * neighbours]).astype(jnp.int32) * piece_count

    backs = []
    asking = queries
    for side in range(2):
        sent = attend(
            side, places, asking, mine, other, mine_bias, other_bias, fresh, fresh_bias, past_rows, heads_here
        )
        asking, sent, backs = lax.optimization_barrier((asking, sent, backs))
        backs = [*backs, lax.all_to_all(sent, "run", 0, 0, tiled=True)]
    columns = []
    for back in backs:
        part = merged(back, head_width).reshape(head_width, heads_here // 2, piece_count)
        columns.append(part.transpose(2, 1, 0).reshape(piece_count, -1))
    attn_rows = jnp.concatenate(
        [jnp.concatenate(columns, axis=1), dec_attn.reshape(dec_count, heads_here * head_width)],
        axis=0,
    ).astype(jnp.bfloat16)
    every_head = jnp.moveaxis(to_each(attn_rows, "tp"), 0, 1).reshape(attn_rows.shape[0], -1)
    mixed = jnp.dot(every_head, w_out, preferred_element_type=jnp.float32).astype(jnp.bfloat16)
    return (mixed[:piece_count], mixed[piece_count:])


def solution(mesh):
    near, core = 4, 2
    grp, kv, tp = (mesh.shape[axis] for axis in ("grp", "kv", "tp"))
    finer = Mesh(
        mesh.devices.reshape(grp, kv // (near * core), near, core, tp),
        ("grp", "run", "near", "core", "tp"),
    )
    return jax.shard_map(
        step,
        mesh=finer,
        in_specs=(
            P(GRP_KV, None),
            P(GRP_KV, None),
            P(),
            P(None, "tp"),
            P(None, "tp"),
            P(None, "tp"),
            P(None, "tp"),
            P("tp"),
            P("tp", GRP_KV),
            P(GRP_KV, "tp", None),
            P("tp", GRP_KV),
            P(GRP_KV, None, "tp", None),
            P(GRP_KV, "tp", None),
            P(GRP_KV),
            P(None, "tp"),
        ),
        out_specs=(P(GRP_KV, "tp"), P(GRP_KV, "tp")),
        check_vma=False,
    )
```

```python
import functools

import jax
import jax.numpy as jnp
from jax import lax
from jax.experimental import pallas as pl
from jax.experimental.pallas import tpu as pltpu
from jax.sharding import Mesh
from jax.sharding import PartitionSpec as P

GRP_KV = ("grp", "run", "near", "core")
PIECES = 3
SPARE = 8


def to_each(array, axis):
    members = lax.axis_size(axis)
    return lax.all_to_all(
        jnp.broadcast_to(array[None], (members, *array.shape)), axis, 0, 0, tiled=True
    )


def norm_rows(rows, gain):
    wide = rows.astype(jnp.float32)
    scale = lax.rsqrt(jnp.mean(wide * wide, axis=-1, keepdims=True) + 1e-06)
    return (wide * scale * gain).astype(jnp.bfloat16)


def absorb(state, score, values):
    peak, acc = state
    highest = jnp.maximum(peak, jnp.max(score, axis=0, keepdims=True))
    weight = jnp.exp(score - highest).astype(jnp.bfloat16)
    fresh = jnp.dot(values, weight, preferred_element_type=jnp.float32)
    return highest, acc * jnp.exp(peak - highest) + fresh


def operands(rows, bias):
    count, width = rows.shape
    half = width // 2
    pieces = bias.shape[0]
    wide = jnp.concatenate(
        [
            jnp.zeros((half, count), jnp.bfloat16),
            bias,
            jnp.zeros((half - pieces, count), jnp.bfloat16),
        ],
        axis=0,
    )
    lane = lax.broadcasted_iota(jnp.int32, (count, width), 1)
    keys = jnp.where(lane < half, rows, wide.T)
    values = jnp.concatenate([rows.T[half:], jnp.ones((16, count), jnp.bfloat16)], axis=0)
    return keys, values


def cut(array):
    first = array.astype(jnp.bfloat16).astype(jnp.float32)
    left = array - first
    second = left.astype(jnp.bfloat16).astype(jnp.float32)
    return [first, second, left - second]


def query_tile(q_ref, first_head, heads):
    members, width, lanes = q_ref.shape
    turned = jnp.concatenate([q_ref[k] for k in range(members)], axis=1)
    each = lanes // (heads // 2)
    shape = (width, members * lanes)
    row = lax.broadcasted_iota(jnp.int32, shape, 0)
    head = first_head + lax.broadcasted_iota(jnp.int32, shape, 1) % lanes // each
    pick = (row % heads == head) & (row < PIECES * heads)
    return jnp.concatenate([turned, pick.astype(jnp.float32).astype(jnp.bfloat16)], axis=0)


def past_kernel(first_head, heads, q_ref, mine_ref, other_ref, mine_bias_ref, other_bias_ref, peak_ref, acc_ref):
    query = query_tile(q_ref, first_head, heads)

    @pl.when(pl.program_id(1) == 0)
    def _():
        peak_ref[...] = jnp.full_like(peak_ref, -jnp.inf)
        acc_ref[...] = jnp.zeros_like(acc_ref)

    state = peak_ref[...], acc_ref[...]
    for kv_ref, bias_ref in ((mine_ref, mine_bias_ref), (other_ref, other_bias_ref)):
        for k in range(kv_ref.shape[0]):
            keys, values = operands(kv_ref[k], bias_ref[k])
            score = jnp.dot(keys, query, preferred_element_type=jnp.float32)
            state = absorb(state, score, values)
    peak_ref[...], acc_ref[...] = state


def fresh_kernel(first_head, heads, place_ref, q_ref, kv_ref, bias_ref, peak_ref, acc_ref, out_ref):
    query = query_tile(q_ref, first_head, heads)
    width, tile = query.shape
    half = width // 2
    members, _, lanes = out_ref.shape
    each = lanes // (heads // 2)
    chunks, count, _ = kv_ref.shape
    state = peak_ref[...], acc_ref[...]
    lane = lax.broadcasted_iota(jnp.int32, (1, tile), 1)
    member = pl.program_id(0) * members + lane // lanes
    asked = member * (chunks * count) + place_ref[0] + lane % each
    for k in range(chunks):
        keys, values = operands(kv_ref[k], bias_ref[k])
        score = jnp.dot(keys, query, preferred_element_type=jnp.float32)
        place = place_ref[1] + k * count + lax.broadcasted_iota(jnp.int32, score.shape, 0)
        score = jnp.where(place <= asked, score, -jnp.inf)
        state = absorb(state, score, values)
    peak, acc = state
    rows = [acc[:half], *cut(peak), *cut(acc[half : half + 1])]
    rows.append(jnp.zeros((SPARE - 2 * PIECES, tile), jnp.float32))
    sent = jnp.concatenate(rows, axis=0).astype(jnp.bfloat16)
    for k in range(members):
        out_ref[k] = sent[:, k * lanes : (k + 1) * lanes]


def attend(side, places, queries, mine, other, mine_bias, other_bias, fresh, fresh_bias, past_rows, heads):
    members, _, lanes = queries.shape
    shards, _, width = mine.shape
    half = width // 2
    at_once, joined = 2, 2
    tile = joined * lanes
    rows = members * lanes
    whole = lambda array: pl.BlockSpec(array.shape, lambda *_: (0,) * array.ndim)
    shard = lambda count: pl.BlockSpec((at_once, count, width), lambda r, s: (s, 0, 0))
    bias_block = pl.BlockSpec((at_once, *mine_bias.shape[1:]), lambda r, s: (s, 0, 0))
    first_head = side * (heads // 2)
    work = 2 * shards * past_rows * rows
    peak, acc = pl.pallas_call(
        functools.partial(past_kernel, first_head, heads),
        grid=(members // joined, shards // at_once),
        in_specs=[
            pl.BlockSpec((joined, half, lanes), lambda r, s: (r, side, 0)),
            shard(past_rows),
            shard(past_rows),
            bias_block,
            bias_block,
        ],
        out_specs=[
            pl.BlockSpec((1, tile), lambda r, s: (0, r)),
            pl.BlockSpec((half + 16, tile), lambda r, s: (0, r)),
        ],
        out_shape=[
            jax.ShapeDtypeStruct((1, rows), jnp.float32),
            jax.ShapeDtypeStruct((half + 16, rows), jnp.float32),
        ],
        compiler_params=pltpu.CompilerParams(
            dimension_semantics=("arbitrary", "arbitrary"), vmem_limit_bytes=40 * 2**20
        ),
        cost_estimate=pl.CostEstimate(
            flops=work * width * 2, transcendentals=work, bytes_accessed=4 * mine.size
        ),
        name="past",
    )(queries, mine, other, mine_bias, other_bias)
    return pl.pallas_call(
        functools.partial(fresh_kernel, first_head, heads),
        grid=(members // joined,),
        in_specs=[
            pl.BlockSpec(memory_space=pltpu.SMEM),
            pl.BlockSpec((joined, half, lanes), lambda r: (r, side, 0)),
            whole(fresh),
            whole(fresh_bias),
            pl.BlockSpec((1, tile), lambda r: (0, r)),
            pl.BlockSpec((half + 16, tile), lambda r: (0, r)),
        ],
        out_specs=pl.BlockSpec((joined, half + SPARE, lanes), lambda r: (r, 0, 0)),
        out_shape=jax.ShapeDtypeStruct((members, half + SPARE, lanes), jnp.bfloat16),
        compiler_params=pltpu.CompilerParams(
            dimension_semantics=("arbitrary",), vmem_limit_bytes=32 * 2**20
        ),
        cost_estimate=pl.CostEstimate(
            flops=fresh.shape[0] * fresh.shape[1] * rows * width * 4,
            transcendentals=fresh.shape[0] * fresh.shape[1] * rows,
            bytes_accessed=4 * acc.size,
        ),
        name="fresh",
    )(places, queries, fresh, fresh_bias, peak, acc)


def bf16_pieces(array, dim):
    first = lax.reduce_precision(array, 8, 7)
    left = array - first
    second = lax.reduce_precision(left, 8, 7)
    return jnp.concatenate([first, second, left - second], axis=dim).astype(jnp.bfloat16)


def bias_rows(bias):
    pieces = bf16_pieces(bias, -2)
    spare = jnp.zeros((*pieces.shape[:-2], 16 - pieces.shape[-2], pieces.shape[-1]), jnp.bfloat16)
    return jnp.concatenate([pieces, spare], axis=-2)


def packed(array, lanes):
    flat = array.reshape(-1)
    rows = -(-flat.shape[0] // lanes)
    return jnp.pad(flat, (0, rows * lanes - flat.shape[0])).reshape(rows, lanes)


def merged(parts, half):
    wide = parts.astype(jnp.float32)
    peak = wide[:, half] + wide[:, half + 1] + wide[:, half + 2]
    total = wide[:, half + 3] + wide[:, half + 4] + wide[:, half + 5]
    share = jnp.exp(peak - jnp.max(peak, axis=0))
    numer = jnp.sum(wide[:, :half] * share[:, None, :], axis=0)
    return numer / jnp.sum(total * share, axis=0)


def decode_attention(query, new_key, new_value, new_gate, cache, gate, lengths):
    seqs, pairs_here, group_size, head_width = query.shape
    span = cache.shape[1]
    keys = cache[..., :head_width]
    values = cache[..., head_width:]
    target_location = jnp.arange(span, dtype=jnp.int32)
    last_gate = jnp.sum(
        jnp.where(target_location[None, None, :] == lengths[:, None, None] - 1, gate, 0.0), axis=-1
    )
    score = jnp.einsum(
        "skgd,slkd->skgl", query, keys, preferred_element_type=jnp.float32
    ) * head_width ** (-0.5)
    score = score - gate.reshape(seqs, pairs_here, group_size, span)
    score = jnp.where(
        (target_location[None, :] < lengths[:, None])[:, None, None, :], score, -jnp.inf
    )
    own = jnp.einsum(
        "skgd,skd->skg", query, new_key, preferred_element_type=jnp.float32
    ) * head_width ** (-0.5)
    own = own - (last_gate + new_gate).reshape(seqs, pairs_here, group_size)
    peak = jnp.maximum(jnp.max(score, axis=-1), own)
    weight = jnp.exp(score - peak[..., None])
    own_weight = jnp.exp(own - peak)
    total = jnp.sum(weight, axis=-1) + own_weight
    numer = jnp.einsum(
        "skgl,slkd->skgd", weight.astype(jnp.bfloat16), values, preferred_element_type=jnp.float32
    )
    numer = numer + own_weight.astype(jnp.bfloat16).astype(jnp.float32)[..., None] * new_value[
        :, :, None, :
    ].astype(jnp.float32)
    return numer / total[..., None]


def step(
    piece_rows,
    dec_rows,
    norm_gain,
    w_query,
    w_key,
    w_value,
    w_forget,
    forget_bias,
    piece_decay,
    cache_kv,
    cache_gate,
    dec_cache,
    dec_gate,
    dec_lengths,
    w_out,
):
    piece_count = piece_rows.shape[0]
    dec_count = dec_rows.shape[0]
    past_rows, pairs_here, width = cache_kv.shape
    head_width = width // 2
    heads_here = w_forget.shape[1]
    group_size = heads_here // pairs_here
    lanes = heads_here // 2 * piece_count
    neighbours = lax.axis_size(("near", "core"))
    me = lax.axis_index(("near", "core"))
    run = lax.axis_index("run")

    past_bias = bias_rows(cache_gate)
    past = jnp.concatenate([cache_kv[:, 0], past_bias.reshape(-1, width)], axis=0)
    mine = to_each(past, "near")

    normed = norm_rows(jnp.concatenate([piece_rows, dec_rows], axis=0), norm_gain)
    query = jnp.dot(normed, w_query, preferred_element_type=jnp.float32).astype(jnp.bfloat16)
    new_key = jnp.dot(normed, w_key, preferred_element_type=jnp.float32).astype(jnp.bfloat16)
    new_value = jnp.dot(normed, w_value, preferred_element_type=jnp.float32).astype(jnp.bfloat16)
    log_gate = jax.nn.log_sigmoid(
        jnp.dot(normed, w_forget, preferred_element_type=jnp.float32) + forget_bias
    )
    running = jnp.cumsum(log_gate[:piece_count].T + piece_decay, axis=1)

    scaled = query[:piece_count] * jnp.asarray(head_width ** (-0.5), query.dtype)
    turned = scaled.reshape(piece_count, 2, heads_here // 2, head_width).transpose(1, 3, 2, 0)
    asked = jnp.concatenate(
        [
            turned.reshape(2 * head_width, lanes),
            packed(bf16_pieces(running[None, :, -1], 0), lanes),
            jnp.zeros((SPARE - 1, lanes), jnp.bfloat16),
        ],
        axis=0,
    )
    queries = lax.all_gather(asked, "run")
    other = lax.ppermute(mine, "core", [(0, 1), (1, 0)])
    mine_bias, other_bias = (
        block[:, past_rows:].reshape(-1, *past_bias.shape) for block in (mine, other)
    )
    totals = queries[:, 2 * head_width, : PIECES * heads_here].astype(jnp.float32)
    totals = totals.reshape(-1, PIECES, heads_here).sum(1)
    earlier = jnp.arange(totals.shape[0], dtype=jnp.int32)[:, None] < run
    earlier = jnp.sum(jnp.where(earlier, totals, 0.0), axis=0)

    own = jnp.concatenate(
        [
            jnp.concatenate([new_key[:piece_count], new_value[:piece_count]], axis=1),
            packed(bf16_pieces(running[None], 0), width),
            packed(bf16_pieces(earlier[None], 0), width),
        ],
        axis=0,
    )
    own = jnp.pad(own, ((0, -own.shape[0] % SPARE), (0, 0)))
    own, _ = lax.optimization_barrier((own, mine))
    news = to_each(own, ("near", "core"))
    run_rows = PIECES * heads_here * piece_count // width
    ran = news[:, piece_count : piece_count + run_rows].astype(jnp.float32)
    ran = ran.reshape(neighbours, PIECES, heads_here, piece_count).sum(1)
    before = news[:, piece_count + run_rows, : PIECES * heads_here].astype(jnp.float32)
    before = before.reshape(neighbours, PIECES, heads_here).sum((0, 1))
    ends = ran[:, :, -1]
    before = before + jnp.cumsum(ends, axis=0) - ends
    joined = 4
    chunks = neighbours // joined
    fresh_bias = -(ran + before[:, :, None])
    fresh_bias = fresh_bias.reshape(chunks, joined, heads_here, piece_count).transpose(0, 2, 1, 3)
    fresh_bias = bias_rows(fresh_bias.reshape(chunks, heads_here, joined * piece_count))
    fresh = news[:, :piece_count].reshape(chunks, joined * piece_count, width)
    places = jnp.stack([me, run * neighbours]).astype(jnp.int32) * piece_count

    backs = []
    asking, dec_query = queries, query[piece_count:]
    for side in range(2):
        sent = attend(
            side, places, asking, mine, other, mine_bias, other_bias, fresh, fresh_bias, past_rows, heads_here
        )
        asking, sent, backs, dec_query = lax.optimization_barrier((asking, sent, backs, dec_query))
        backs = [*backs, lax.all_to_all(sent, "run", 0, 0, tiled=True)]
    dec_attn = decode_attention(
        dec_query.reshape(dec_count, pairs_here, group_size, head_width),
        new_key[piece_count:].reshape(dec_count, pairs_here, head_width),
        new_value[piece_count:].reshape(dec_count, pairs_here, head_width),
        log_gate[piece_count:],
        dec_cache,
        dec_gate,
        dec_lengths,
    )
    columns = []
    for back in backs:
        part = merged(back, head_width).reshape(head_width, heads_here // 2, piece_count)
        columns.append(part.transpose(2, 1, 0).reshape(piece_count, -1))
    attn_rows = jnp.concatenate(
        [jnp.concatenate(columns, axis=1), dec_attn.reshape(dec_count, heads_here * head_width)],
        axis=0,
    ).astype(jnp.bfloat16)
    every_head = jnp.moveaxis(to_each(attn_rows, "tp"), 0, 1).reshape(attn_rows.shape[0], -1)
    mixed = jnp.dot(every_head, w_out, preferred_element_type=jnp.float32).astype(jnp.bfloat16)
    return (mixed[:piece_count], mixed[piece_count:])


def solution(mesh):
    near, core = 4, 2
    grp, kv, tp = (mesh.shape[axis] for axis in ("grp", "kv", "tp"))
    finer = Mesh(
        mesh.devices.reshape(grp, kv // (near * core), near, core, tp),
        ("grp", "run", "near", "core", "tp"),
    )
    return jax.shard_map(
        step,
        mesh=finer,
        in_specs=(
            P(GRP_KV, None),
            P(GRP_KV, None),
            P(),
            P(None, "tp"),
            P(None, "tp"),
            P(None, "tp"),
            P(None, "tp"),
            P("tp"),
            P("tp", GRP_KV),
            P(GRP_KV, "tp", None),
            P("tp", GRP_KV),
            P(GRP_KV, None, "tp", None),
            P(GRP_KV, "tp", None),
            P(GRP_KV),
            P(None, "tp"),
        ),
        out_specs=(P(GRP_KV, "tp"), P(GRP_KV, "tp")),
        check_vma=False,
    )
```

```python
import functools

import jax
import jax.numpy as jnp
from jax import lax
from jax.experimental import pallas as pl
from jax.experimental.pallas import tpu as pltpu
from jax.sharding import Mesh
from jax.sharding import PartitionSpec as P

GRP_KV = ("grp", "run", "near", "core")
PIECES = 3
SPARE = 8
AT_ONCE = 4
JOINED = 4


def to_each(array, axis):
    members = lax.axis_size(axis)
    return lax.all_to_all(
        jnp.broadcast_to(array[None], (members, *array.shape)), axis, 0, 0, tiled=True
    )


def norm_rows(rows, gain):
    wide = rows.astype(jnp.float32)
    scale = lax.rsqrt(jnp.mean(wide * wide, axis=-1, keepdims=True) + 1e-06)
    return (wide * scale * gain).astype(jnp.bfloat16)


def absorb(state, score, values):
    peak, acc = state
    highest = jnp.maximum(peak, jnp.max(score, axis=0, keepdims=True))
    weight = jnp.exp(score - highest).astype(jnp.bfloat16)
    fresh = jnp.dot(values, weight, preferred_element_type=jnp.float32)
    return highest, acc * jnp.exp(peak - highest) + fresh


def operands(rows, bias):
    count, width = rows.shape
    half = width // 2
    pieces = bias.shape[0]
    wide = jnp.concatenate(
        [
            jnp.zeros((half, count), jnp.bfloat16),
            bias,
            jnp.zeros((half - pieces, count), jnp.bfloat16),
        ],
        axis=0,
    )
    lane = lax.broadcasted_iota(jnp.int32, (count, width), 1)
    keys = jnp.where(lane < half, rows, wide.T)
    values = jnp.concatenate([rows.T[half:], jnp.ones((16, count), jnp.bfloat16)], axis=0)
    return keys, values


def cut(array):
    first = array.astype(jnp.bfloat16).astype(jnp.float32)
    left = array - first
    second = left.astype(jnp.bfloat16).astype(jnp.float32)
    return [first, second, left - second]


def query_tile(q_ref, heads):
    members, width, lanes = q_ref.shape
    turned = jnp.concatenate([q_ref[k] for k in range(members)], axis=1)
    each = lanes // heads
    shape = (width, members * lanes)
    row = lax.broadcasted_iota(jnp.int32, shape, 0)
    head = lax.broadcasted_iota(jnp.int32, shape, 1) % lanes // each
    pick = (row % heads == head) & (row < PIECES * heads)
    return jnp.concatenate([turned, pick.astype(jnp.float32).astype(jnp.bfloat16)], axis=0)


def past_kernel(heads, q_ref, mine_ref, other_ref, mine_bias_ref, other_bias_ref, peak_ref, acc_ref):
    query = query_tile(q_ref, heads)

    @pl.when(pl.program_id(1) == 0)
    def _():
        peak_ref[...] = jnp.full_like(peak_ref, -jnp.inf)
        acc_ref[...] = jnp.zeros_like(acc_ref)

    state = peak_ref[...], acc_ref[...]
    for kv_ref, bias_ref in ((mine_ref, mine_bias_ref), (other_ref, other_bias_ref)):
        for k in range(kv_ref.shape[0]):
            keys, values = operands(kv_ref[k], bias_ref[k])
            score = jnp.dot(keys, query, preferred_element_type=jnp.float32)
            state = absorb(state, score, values)
    peak_ref[...], acc_ref[...] = state


def fresh_kernel(heads, place_ref, q_ref, kv_ref, bias_ref, peak_ref, acc_ref, out_ref):
    query = query_tile(q_ref, heads)
    width, tile = query.shape
    half = width // 2
    members, _, lanes = out_ref.shape
    each = lanes // heads
    chunks, count, _ = kv_ref.shape
    state = peak_ref[...], acc_ref[...]
    lane = lax.broadcasted_iota(jnp.int32, (1, tile), 1)
    member = pl.program_id(0) * members + lane // lanes
    asked = member * (chunks * count) + place_ref[0] + lane % each
    for k in range(chunks):
        keys, values = operands(kv_ref[k], bias_ref[k])
        score = jnp.dot(keys, query, preferred_element_type=jnp.float32)
        place = place_ref[1] + k * count + lax.broadcasted_iota(jnp.int32, score.shape, 0)
        score = jnp.where(place <= asked, score, -jnp.inf)
        state = absorb(state, score, values)
    peak, acc = state
    rows = [acc[:half], *cut(peak), *cut(acc[half : half + 1])]
    rows.append(jnp.zeros((SPARE - 2 * PIECES, tile), jnp.float32))
    sent = jnp.concatenate(rows, axis=0).astype(jnp.bfloat16)
    for k in range(members):
        out_ref[k] = sent[:, k * lanes : (k + 1) * lanes]


def attend(places, queries, mine, other, mine_bias, other_bias, fresh, fresh_bias, past_rows, heads):
    members, _, lanes = queries.shape
    shards, _, width = mine.shape
    half = width // 2
    at_once, joined = AT_ONCE, JOINED
    tile = joined * lanes
    rows = members * lanes
    whole = lambda array: pl.BlockSpec(array.shape, lambda *_: (0,) * array.ndim)
    shard = lambda count: pl.BlockSpec((at_once, count, width), lambda r, s: (s, 0, 0))
    bias_block = pl.BlockSpec((at_once, *mine_bias.shape[1:]), lambda r, s: (s, 0, 0))
    work = 2 * shards * past_rows * rows
    peak, acc = pl.pallas_call(
        functools.partial(past_kernel, heads),
        grid=(members // joined, shards // at_once),
        in_specs=[
            pl.BlockSpec((joined, half, lanes), lambda r, s: (r, 0, 0)),
            shard(past_rows),
            shard(past_rows),
            bias_block,
            bias_block,
        ],
        out_specs=[
            pl.BlockSpec((1, tile), lambda r, s: (0, r)),
            pl.BlockSpec((half + 16, tile), lambda r, s: (0, r)),
        ],
        out_shape=[
            jax.ShapeDtypeStruct((1, rows), jnp.float32),
            jax.ShapeDtypeStruct((half + 16, rows), jnp.float32),
        ],
        compiler_params=pltpu.CompilerParams(
            dimension_semantics=("arbitrary", "arbitrary"), vmem_limit_bytes=40 * 2**20
        ),
        cost_estimate=pl.CostEstimate(
            flops=work * width * 2, transcendentals=work, bytes_accessed=4 * mine.size
        ),
        name="past",
    )(queries, mine, other, mine_bias, other_bias)
    return pl.pallas_call(
        functools.partial(fresh_kernel, heads),
        grid=(members // joined,),
        in_specs=[
            pl.BlockSpec(memory_space=pltpu.SMEM),
            pl.BlockSpec((joined, half, lanes), lambda r: (r, 0, 0)),
            whole(fresh),
            whole(fresh_bias),
            pl.BlockSpec((1, tile), lambda r: (0, r)),
            pl.BlockSpec((half + 16, tile), lambda r: (0, r)),
        ],
        out_specs=pl.BlockSpec((joined, half + SPARE, lanes), lambda r: (r, 0, 0)),
        out_shape=jax.ShapeDtypeStruct((members, half + SPARE, lanes), jnp.bfloat16),
        compiler_params=pltpu.CompilerParams(
            dimension_semantics=("arbitrary",), vmem_limit_bytes=32 * 2**20
        ),
        cost_estimate=pl.CostEstimate(
            flops=fresh.shape[0] * fresh.shape[1] * rows * width * 4,
            transcendentals=fresh.shape[0] * fresh.shape[1] * rows,
            bytes_accessed=4 * acc.size,
        ),
        name="fresh",
    )(places, queries, fresh, fresh_bias, peak, acc)


def bf16_pieces(array, dim):
    first = lax.reduce_precision(array, 8, 7)
    left = array - first
    second = lax.reduce_precision(left, 8, 7)
    return jnp.concatenate([first, second, left - second], axis=dim).astype(jnp.bfloat16)


def bias_rows(bias):
    pieces = bf16_pieces(bias, -2)
    spare = jnp.zeros((*pieces.shape[:-2], 16 - pieces.shape[-2], pieces.shape[-1]), jnp.bfloat16)
    return jnp.concatenate([pieces, spare], axis=-2)


def packed(array, lanes):
    flat = array.reshape(-1)
    rows = -(-flat.shape[0] // lanes)
    return jnp.pad(flat, (0, rows * lanes - flat.shape[0])).reshape(rows, lanes)


def merged(parts, half):
    wide = parts.astype(jnp.float32)
    peak = wide[:, half] + wide[:, half + 1] + wide[:, half + 2]
    total = wide[:, half + 3] + wide[:, half + 4] + wide[:, half + 5]
    share = jnp.exp(peak - jnp.max(peak, axis=0))
    numer = jnp.sum(wide[:, :half] * share[:, None, :], axis=0)
    return numer / jnp.sum(total * share, axis=0)


def decode_attention(query, new_key, new_value, new_gate, cache, gate, lengths):
    seqs, pairs_here, group_size, head_width = query.shape
    span = cache.shape[1]
    keys = cache[..., :head_width]
    values = cache[..., head_width:]
    target_location = jnp.arange(span, dtype=jnp.int32)
    last_gate = jnp.sum(
        jnp.where(target_location[None, None, :] == lengths[:, None, None] - 1, gate, 0.0), axis=-1
    )
    score = jnp.einsum(
        "skgd,slkd->skgl", query, keys, preferred_element_type=jnp.float32
    ) * head_width ** (-0.5)
    score = score - gate.reshape(seqs, pairs_here, group_size, span)
    score = jnp.where(
        (target_location[None, :] < lengths[:, None])[:, None, None, :], score, -jnp.inf
    )
    own = jnp.einsum(
        "skgd,skd->skg", query, new_key, preferred_element_type=jnp.float32
    ) * head_width ** (-0.5)
    own = own - (last_gate + new_gate).reshape(seqs, pairs_here, group_size)
    peak = jnp.maximum(jnp.max(score, axis=-1), own)
    weight = jnp.exp(score - peak[..., None])
    own_weight = jnp.exp(own - peak)
    total = jnp.sum(weight, axis=-1) + own_weight
    numer = jnp.einsum(
        "skgl,slkd->skgd", weight.astype(jnp.bfloat16), values, preferred_element_type=jnp.float32
    )
    numer = numer + own_weight.astype(jnp.bfloat16).astype(jnp.float32)[..., None] * new_value[
        :, :, None, :
    ].astype(jnp.float32)
    return numer / total[..., None]


def step(
    piece_rows,
    dec_rows,
    norm_gain,
    w_query,
    w_key,
    w_value,
    w_forget,
    forget_bias,
    piece_decay,
    cache_kv,
    cache_gate,
    dec_cache,
    dec_gate,
    dec_lengths,
    w_out,
):
    piece_count = piece_rows.shape[0]
    dec_count = dec_rows.shape[0]
    past_rows, pairs_here, width = cache_kv.shape
    head_width = width // 2
    heads_here = w_forget.shape[1]
    group_size = heads_here // pairs_here
    lanes = heads_here * piece_count
    neighbours = lax.axis_size(("near", "core"))
    me = lax.axis_index(("near", "core"))
    run = lax.axis_index("run")

    past_bias = bias_rows(cache_gate)
    past = jnp.concatenate([cache_kv[:, 0], past_bias.reshape(-1, width)], axis=0)
    mine = to_each(past, "near")

    normed = norm_rows(jnp.concatenate([piece_rows, dec_rows], axis=0), norm_gain)
    query = jnp.dot(normed, w_query, preferred_element_type=jnp.float32).astype(jnp.bfloat16)
    new_key = jnp.dot(normed, w_key, preferred_element_type=jnp.float32).astype(jnp.bfloat16)
    new_value = jnp.dot(normed, w_value, preferred_element_type=jnp.float32).astype(jnp.bfloat16)
    log_gate = jax.nn.log_sigmoid(
        jnp.dot(normed, w_forget, preferred_element_type=jnp.float32) + forget_bias
    )
    running = jnp.cumsum(log_gate[:piece_count].T + piece_decay, axis=1)

    scaled = query[:piece_count] * jnp.asarray(head_width ** (-0.5), query.dtype)
    turned = scaled.reshape(piece_count, heads_here, head_width).transpose(2, 1, 0)
    asked = jnp.concatenate(
        [
            turned.reshape(head_width, lanes),
            packed(bf16_pieces(running[None, :, -1], 0), lanes),
            jnp.zeros((SPARE - 1, lanes), jnp.bfloat16),
        ],
        axis=0,
    )
    queries = lax.all_gather(asked, "run")
    other = lax.ppermute(mine, "core", [(0, 1), (1, 0)])
    mine_bias, other_bias = (
        block[:, past_rows:].reshape(-1, *past_bias.shape) for block in (mine, other)
    )
    totals = queries[:, head_width, : PIECES * heads_here].astype(jnp.float32)
    totals = totals.reshape(-1, PIECES, heads_here).sum(1)
    earlier = jnp.arange(totals.shape[0], dtype=jnp.int32)[:, None] < run
    earlier = jnp.sum(jnp.where(earlier, totals, 0.0), axis=0)

    own = jnp.concatenate(
        [
            jnp.concatenate([new_key[:piece_count], new_value[:piece_count]], axis=1),
            packed(bf16_pieces(running[None], 0), width),
            packed(bf16_pieces(earlier[None], 0), width),
        ],
        axis=0,
    )
    own = jnp.pad(own, ((0, -own.shape[0] % SPARE), (0, 0)))
    own, _ = lax.optimization_barrier((own, mine))
    news = to_each(own, ("near", "core"))
    run_rows = PIECES * heads_here * piece_count // width
    ran = news[:, piece_count : piece_count + run_rows].astype(jnp.float32)
    ran = ran.reshape(neighbours, PIECES, heads_here, piece_count).sum(1)
    before = news[:, piece_count + run_rows, : PIECES * heads_here].astype(jnp.float32)
    before = before.reshape(neighbours, PIECES, heads_here).sum((0, 1))
    ends = ran[:, :, -1]
    before = before + jnp.cumsum(ends, axis=0) - ends
    joined = 4
    chunks = neighbours // joined
    fresh_bias = -(ran + before[:, :, None])
    fresh_bias = fresh_bias.reshape(chunks, joined, heads_here, piece_count).transpose(0, 2, 1, 3)
    fresh_bias = bias_rows(fresh_bias.reshape(chunks, heads_here, joined * piece_count))
    fresh = news[:, :piece_count].reshape(chunks, joined * piece_count, width)
    places = jnp.stack([me, run * neighbours]).astype(jnp.int32) * piece_count

    sent = attend(
        places, queries, mine, other, mine_bias, other_bias, fresh, fresh_bias, past_rows, heads_here
    )
    sent, dec_query = lax.optimization_barrier((sent, query[piece_count:]))
    back = lax.all_to_all(sent, "run", 0, 0, tiled=True)
    dec_attn = decode_attention(
        dec_query.reshape(dec_count, pairs_here, group_size, head_width),
        new_key[piece_count:].reshape(dec_count, pairs_here, head_width),
        new_value[piece_count:].reshape(dec_count, pairs_here, head_width),
        log_gate[piece_count:],
        dec_cache,
        dec_gate,
        dec_lengths,
    )
    piece_attn = merged(back, head_width).reshape(head_width, heads_here, piece_count)
    piece_attn = piece_attn.transpose(2, 1, 0).reshape(piece_count, -1)
    attn_rows = jnp.concatenate(
        [piece_attn, dec_attn.reshape(dec_count, heads_here * head_width)],
        axis=0,
    ).astype(jnp.bfloat16)
    every_head = jnp.moveaxis(to_each(attn_rows, "tp"), 0, 1).reshape(attn_rows.shape[0], -1)
    mixed = jnp.dot(every_head, w_out, preferred_element_type=jnp.float32).astype(jnp.bfloat16)
    return (mixed[:piece_count], mixed[piece_count:])


def solution(mesh):
    near, core = 4, 2
    grp, kv, tp = (mesh.shape[axis] for axis in ("grp", "kv", "tp"))
    finer = Mesh(
        mesh.devices.reshape(grp, kv // (near * core), near, core, tp),
        ("grp", "run", "near", "core", "tp"),
    )
    return jax.shard_map(
        step,
        mesh=finer,
        in_specs=(
            P(GRP_KV, None),
            P(GRP_KV, None),
            P(),
            P(None, "tp"),
            P(None, "tp"),
            P(None, "tp"),
            P(None, "tp"),
            P("tp"),
            P("tp", GRP_KV),
            P(GRP_KV, "tp", None),
            P("tp", GRP_KV),
            P(GRP_KV, None, "tp", None),
            P(GRP_KV, "tp", None),
            P(GRP_KV),
            P(None, "tp"),
        ),
        out_specs=(P(GRP_KV, "tp"), P(GRP_KV, "tp")),
        check_vma=False,
    )
```

```python
import functools

import jax
import jax.numpy as jnp
from jax import lax
from jax.experimental import pallas as pl
from jax.experimental.pallas import tpu as pltpu
from jax.sharding import Mesh
from jax.sharding import PartitionSpec as P

GRP_KV = ("grp", "run", "near", "core")
PIECES = 3
SPARE = 8
AT_ONCE = 4
JOINED = 8


def to_each(array, axis):
    members = lax.axis_size(axis)
    return lax.all_to_all(
        jnp.broadcast_to(array[None], (members, *array.shape)), axis, 0, 0, tiled=True
    )


def norm_rows(rows, gain):
    wide = rows.astype(jnp.float32)
    scale = lax.rsqrt(jnp.mean(wide * wide, axis=-1, keepdims=True) + 1e-06)
    return (wide * scale * gain).astype(jnp.bfloat16)


def absorb(state, score, values):
    peak, acc = state
    highest = jnp.maximum(peak, jnp.max(score, axis=0, keepdims=True))
    weight = jnp.exp(score - highest).astype(jnp.bfloat16)
    fresh = jnp.dot(values, weight, preferred_element_type=jnp.float32)
    return highest, acc * jnp.exp(peak - highest) + fresh


def operands(rows, bias):
    count, width = rows.shape
    half = width // 2
    pieces = bias.shape[0]
    wide = jnp.concatenate(
        [
            jnp.zeros((half, count), jnp.bfloat16),
            bias,
            jnp.zeros((half - pieces, count), jnp.bfloat16),
        ],
        axis=0,
    )
    lane = lax.broadcasted_iota(jnp.int32, (count, width), 1)
    keys = jnp.where(lane < half, rows, wide.T)
    values = jnp.concatenate([rows.T[half:], jnp.ones((16, count), jnp.bfloat16)], axis=0)
    return keys, values


def cut(array):
    first = array.astype(jnp.bfloat16).astype(jnp.float32)
    left = array - first
    second = left.astype(jnp.bfloat16).astype(jnp.float32)
    return [first, second, left - second]


def query_tile(q_ref, heads):
    members, width, lanes = q_ref.shape
    turned = jnp.concatenate([q_ref[k] for k in range(members)], axis=1)
    each = lanes // heads
    shape = (width, members * lanes)
    row = lax.broadcasted_iota(jnp.int32, shape, 0)
    head = lax.broadcasted_iota(jnp.int32, shape, 1) % lanes // each
    pick = (row % heads == head) & (row < PIECES * heads)
    return jnp.concatenate([turned, pick.astype(jnp.float32).astype(jnp.bfloat16)], axis=0)


def past_kernel(heads, past_rows, q_ref, mine_ref, other_ref, peak_ref, acc_ref):
    query = query_tile(q_ref, heads)

    @pl.when(pl.program_id(1) == 0)
    def _():
        peak_ref[...] = jnp.full_like(peak_ref, -jnp.inf)
        acc_ref[...] = jnp.zeros_like(acc_ref)

    state = peak_ref[...], acc_ref[...]
    for kv_ref in (mine_ref, other_ref):
        shards, count, lanes = kv_ref.shape
        pieces = (count - past_rows) // (past_rows // lanes)
        for k in range(shards):
            starts = range(past_rows, count, pieces)
            bias = jnp.concatenate([kv_ref[k, j : j + pieces] for j in starts], axis=1)
            keys, values = operands(kv_ref[k, :past_rows], bias)
            score = jnp.dot(keys, query, preferred_element_type=jnp.float32)
            state = absorb(state, score, values)
    peak_ref[...], acc_ref[...] = state


def fresh_kernel(heads, place_ref, q_ref, kv_ref, bias_ref, peak_ref, acc_ref, out_ref):
    query = query_tile(q_ref, heads)
    width, tile = query.shape
    half = width // 2
    members, _, lanes = out_ref.shape
    each = lanes // heads
    chunks, count, _ = kv_ref.shape
    state = peak_ref[...], acc_ref[...]
    lane = lax.broadcasted_iota(jnp.int32, (1, tile), 1)
    member = pl.program_id(0) * members + lane // lanes
    asked = member * (chunks * count) + place_ref[0] + lane % each
    for k in range(chunks):
        keys, values = operands(kv_ref[k], bias_ref[k])
        score = jnp.dot(keys, query, preferred_element_type=jnp.float32)
        place = place_ref[1] + k * count + lax.broadcasted_iota(jnp.int32, score.shape, 0)
        score = jnp.where(place <= asked, score, -jnp.inf)
        state = absorb(state, score, values)
    peak, acc = state
    rows = [acc[:half], *cut(peak), *cut(acc[half : half + 1])]
    rows.append(jnp.zeros((SPARE - 2 * PIECES, tile), jnp.float32))
    sent = jnp.concatenate(rows, axis=0).astype(jnp.bfloat16)
    for k in range(members):
        out_ref[k] = sent[:, k * lanes : (k + 1) * lanes]


def attend(places, queries, mine, other, fresh, fresh_bias, past_rows, heads):
    members, _, lanes = queries.shape
    shards, past_count, width = mine.shape
    half = width // 2
    at_once, joined = AT_ONCE, JOINED
    tile = joined * lanes
    rows = members * lanes
    whole = lambda array: pl.BlockSpec(array.shape, lambda *_: (0,) * array.ndim)
    shard = pl.BlockSpec((at_once, past_count, width), lambda r, s: (s, 0, 0))
    work = 2 * shards * past_rows * rows
    peak, acc = pl.pallas_call(
        functools.partial(past_kernel, heads, past_rows),
        grid=(members // joined, shards // at_once),
        in_specs=[
            pl.BlockSpec((joined, half, lanes), lambda r, s: (r, 0, 0)),
            shard,
            shard,
        ],
        out_specs=[
            pl.BlockSpec((1, tile), lambda r, s: (0, r)),
            pl.BlockSpec((half + 16, tile), lambda r, s: (0, r)),
        ],
        out_shape=[
            jax.ShapeDtypeStruct((1, rows), jnp.float32),
            jax.ShapeDtypeStruct((half + 16, rows), jnp.float32),
        ],
        compiler_params=pltpu.CompilerParams(
            dimension_semantics=("arbitrary", "arbitrary"), vmem_limit_bytes=32 * 2**20
        ),
        cost_estimate=pl.CostEstimate(
            flops=work * width * 2, transcendentals=work, bytes_accessed=4 * mine.size
        ),
        name="past",
    )(queries, mine, other)
    return pl.pallas_call(
        functools.partial(fresh_kernel, heads),
        grid=(members // joined,),
        in_specs=[
            pl.BlockSpec(memory_space=pltpu.SMEM),
            pl.BlockSpec((joined, half, lanes), lambda r: (r, 0, 0)),
            whole(fresh),
            whole(fresh_bias),
            pl.BlockSpec((1, tile), lambda r: (0, r)),
            pl.BlockSpec((half + 16, tile), lambda r: (0, r)),
        ],
        out_specs=pl.BlockSpec((joined, half + SPARE, lanes), lambda r: (r, 0, 0)),
        out_shape=jax.ShapeDtypeStruct((members, half + SPARE, lanes), jnp.bfloat16),
        compiler_params=pltpu.CompilerParams(
            dimension_semantics=("arbitrary",), vmem_limit_bytes=16 * 2**20
        ),
        cost_estimate=pl.CostEstimate(
            flops=fresh.shape[0] * fresh.shape[1] * rows * width * 4,
            transcendentals=fresh.shape[0] * fresh.shape[1] * rows,
            bytes_accessed=4 * acc.size,
        ),
        name="fresh",
    )(places, queries, fresh, fresh_bias, peak, acc)


def bf16_pieces(array, dim):
    first = lax.reduce_precision(array, 8, 7)
    left = array - first
    second = lax.reduce_precision(left, 8, 7)
    return jnp.concatenate([first, second, left - second], axis=dim).astype(jnp.bfloat16)


def bias_rows(bias):
    pieces = bf16_pieces(bias, -2)
    spare = jnp.zeros((*pieces.shape[:-2], 16 - pieces.shape[-2], pieces.shape[-1]), jnp.bfloat16)
    return jnp.concatenate([pieces, spare], axis=-2)


def packed(array, lanes):
    flat = array.reshape(-1)
    rows = -(-flat.shape[0] // lanes)
    return jnp.pad(flat, (0, rows * lanes - flat.shape[0])).reshape(rows, lanes)


def merged(parts, half):
    wide = parts.astype(jnp.float32)
    peak = wide[:, half] + wide[:, half + 1] + wide[:, half + 2]
    total = wide[:, half + 3] + wide[:, half + 4] + wide[:, half + 5]
    share = jnp.exp(peak - jnp.max(peak, axis=0))
    numer = jnp.sum(wide[:, :half] * share[:, None, :], axis=0)
    return numer / jnp.sum(total * share, axis=0)


def decode_attention(query, new_key, new_value, new_gate, cache, gate, lengths):
    seqs, pairs_here, group_size, head_width = query.shape
    span = cache.shape[1]
    keys = cache[..., :head_width]
    values = cache[..., head_width:]
    target_location = jnp.arange(span, dtype=jnp.int32)
    last_gate = jnp.sum(
        jnp.where(target_location[None, None, :] == lengths[:, None, None] - 1, gate, 0.0), axis=-1
    )
    score = jnp.einsum(
        "skgd,slkd->skgl", query, keys, preferred_element_type=jnp.float32
    ) * head_width ** (-0.5)
    score = score - gate.reshape(seqs, pairs_here, group_size, span)
    score = jnp.where(
        (target_location[None, :] < lengths[:, None])[:, None, None, :], score, -jnp.inf
    )
    own = jnp.einsum(
        "skgd,skd->skg", query, new_key, preferred_element_type=jnp.float32
    ) * head_width ** (-0.5)
    own = own - (last_gate + new_gate).reshape(seqs, pairs_here, group_size)
    peak = jnp.maximum(jnp.max(score, axis=-1), own)
    weight = jnp.exp(score - peak[..., None])
    own_weight = jnp.exp(own - peak)
    total = jnp.sum(weight, axis=-1) + own_weight
    numer = jnp.einsum(
        "skgl,slkd->skgd", weight.astype(jnp.bfloat16), values, preferred_element_type=jnp.float32
    )
    numer = numer + own_weight.astype(jnp.bfloat16).astype(jnp.float32)[..., None] * new_value[
        :, :, None, :
    ].astype(jnp.float32)
    return numer / total[..., None]


def step(
    piece_rows,
    dec_rows,
    norm_gain,
    w_query,
    w_key,
    w_value,
    w_forget,
    forget_bias,
    piece_decay,
    cache_kv,
    cache_gate,
    dec_cache,
    dec_gate,
    dec_lengths,
    w_out,
):
    piece_count = piece_rows.shape[0]
    dec_count = dec_rows.shape[0]
    past_rows, pairs_here, width = cache_kv.shape
    head_width = width // 2
    heads_here = w_forget.shape[1]
    group_size = heads_here // pairs_here
    lanes = heads_here * piece_count
    neighbours = lax.axis_size(("near", "core"))
    me = lax.axis_index(("near", "core"))
    run = lax.axis_index("run")

    past_bias = bias_rows(cache_gate)
    past_bias = past_bias.reshape(past_bias.shape[0], -1, width).transpose(1, 0, 2)
    past = jnp.concatenate([cache_kv[:, 0], past_bias.reshape(-1, width)], axis=0)
    mine = to_each(past, "near")

    normed = norm_rows(jnp.concatenate([piece_rows, dec_rows], axis=0), norm_gain)
    query = jnp.dot(normed, w_query, preferred_element_type=jnp.float32).astype(jnp.bfloat16)
    new_key = jnp.dot(normed, w_key, preferred_element_type=jnp.float32).astype(jnp.bfloat16)
    new_value = jnp.dot(normed, w_value, preferred_element_type=jnp.float32).astype(jnp.bfloat16)
    log_gate = jax.nn.log_sigmoid(
        jnp.dot(normed, w_forget, preferred_element_type=jnp.float32) + forget_bias
    )
    running = jnp.cumsum(log_gate[:piece_count].T + piece_decay, axis=1)

    scaled = query[:piece_count] * jnp.asarray(head_width ** (-0.5), query.dtype)
    turned = scaled.reshape(piece_count, heads_here, head_width).transpose(2, 1, 0)
    asked = jnp.concatenate(
        [
            turned.reshape(head_width, lanes),
            packed(bf16_pieces(running[None, :, -1], 0), lanes),
            jnp.zeros((SPARE - 1, lanes), jnp.bfloat16),
        ],
        axis=0,
    )
    asked, mine = lax.optimization_barrier((asked, mine))
    other = lax.ppermute(mine, "core", [(0, 1), (1, 0)])
    queries = lax.all_gather(asked, "run")
    totals = queries[:, head_width, : PIECES * heads_here].astype(jnp.float32)
    totals = totals.reshape(-1, PIECES, heads_here).sum(1)
    earlier = jnp.arange(totals.shape[0], dtype=jnp.int32)[:, None] < run
    earlier = jnp.sum(jnp.where(earlier, totals, 0.0), axis=0)

    own = jnp.concatenate(
        [
            jnp.concatenate([new_key[:piece_count], new_value[:piece_count]], axis=1),
            packed(bf16_pieces(running[None], 0), width),
            packed(bf16_pieces(earlier[None], 0), width),
        ],
        axis=0,
    )
    own = jnp.pad(own, ((0, -own.shape[0] % SPARE), (0, 0)))
    own, _ = lax.optimization_barrier((own, mine))
    news = to_each(own, ("near", "core"))
    run_rows = PIECES * heads_here * piece_count // width
    ran = news[:, piece_count : piece_count + run_rows].astype(jnp.float32)
    ran = ran.reshape(neighbours, PIECES, heads_here, piece_count).sum(1)
    before = news[:, piece_count + run_rows, : PIECES * heads_here].astype(jnp.float32)
    before = before.reshape(neighbours, PIECES, heads_here).sum((0, 1))
    ends = ran[:, :, -1]
    before = before + jnp.cumsum(ends, axis=0) - ends
    joined = 4
    chunks = neighbours // joined
    fresh_bias = -(ran + before[:, :, None])
    fresh_bias = fresh_bias.reshape(chunks, joined, heads_here, piece_count).transpose(0, 2, 1, 3)
    fresh_bias = bias_rows(fresh_bias.reshape(chunks, heads_here, joined * piece_count))
    fresh = news[:, :piece_count].reshape(chunks, joined * piece_count, width)
    places = jnp.stack([me, run * neighbours]).astype(jnp.int32) * piece_count

    sent = attend(
        places, queries, mine, other, fresh, fresh_bias, past_rows, heads_here
    )
    sent, dec_query = lax.optimization_barrier((sent, query[piece_count:]))
    back = lax.all_to_all(sent, "run", 0, 0, tiled=True)
    dec_attn = decode_attention(
        dec_query.reshape(dec_count, pairs_here, group_size, head_width),
        new_key[piece_count:].reshape(dec_count, pairs_here, head_width),
        new_value[piece_count:].reshape(dec_count, pairs_here, head_width),
        log_gate[piece_count:],
        dec_cache,
        dec_gate,
        dec_lengths,
    )
    piece_attn = merged(back, head_width).reshape(head_width, heads_here, piece_count)
    piece_attn = piece_attn.transpose(2, 1, 0).reshape(piece_count, -1)
    attn_rows = jnp.concatenate(
        [piece_attn, dec_attn.reshape(dec_count, heads_here * head_width)],
        axis=0,
    ).astype(jnp.bfloat16)
    every_head = jnp.moveaxis(to_each(attn_rows, "tp"), 0, 1).reshape(attn_rows.shape[0], -1)
    return tuple(
        jnp.dot(rows, w_out, preferred_element_type=jnp.float32).astype(jnp.bfloat16)
        for rows in (every_head[:piece_count], every_head[piece_count:])
    )


def solution(mesh):
    near, core = 4, 2
    grp, kv, tp = (mesh.shape[axis] for axis in ("grp", "kv", "tp"))
    finer = Mesh(
        mesh.devices.reshape(grp, kv // (near * core), near, core, tp),
        ("grp", "run", "near", "core", "tp"),
    )
    return jax.shard_map(
        step,
        mesh=finer,
        in_specs=(
            P(GRP_KV, None),
            P(GRP_KV, None),
            P(),
            P(None, "tp"),
            P(None, "tp"),
            P(None, "tp"),
            P(None, "tp"),
            P("tp"),
            P("tp", GRP_KV),
            P(GRP_KV, "tp", None),
            P("tp", GRP_KV),
            P(GRP_KV, None, "tp", None),
            P(GRP_KV, "tp", None),
            P(GRP_KV),
            P(None, "tp"),
        ),
        out_specs=(P(GRP_KV, "tp"), P(GRP_KV, "tp")),
        check_vma=False,
    )
```
